32 devices in a mesh: sp: 8 (over z, y), tp: 4 (over x, core).
Axes of the slice: x: 2, y: 2, z: 4, core: 2. Of those that a mesh axis runs over, the one named last changes fastest.
Arguments:
- tokens: bfloat16 [4, 512, 1024], P(None, 'sp', 'tp'), may hold values from -6 to 6
- norm_gain: float32 [4, 1024], replicated, may hold values from 0.1 to 1.9
- val_weight: bfloat16 [4, 1024, 512], P(None, 'sp', 'tp'), may hold values from -0.1875 to 0.1875
- gate_weight: bfloat16 [4, 1024, 512], P(None, 'sp', 'tp'), may hold values from -0.1875 to 0.1875
- conv_taps: float32 [4, 31, 512], P(None, None, 'tp'), may hold values from -1 to 1
- conv_bias: float32 [4, 512], P(None, 'tp'), may hold values from -3 to 3
- ln_gain: float32 [4, 512], P(None, 'tp'), may hold values from 0.1 to 1.9
- ln_shift: float32 [4, 512], P(None, 'tp'), may hold values from -3 to 3
- out_weight: bfloat16 [4, 512, 1024], P(None, 'tp', 'sp'), may hold values from -0.25 to 0.25
Outputs:
- stream: bfloat16 [4, 512, 1024], P(None, 'sp', 'tp')
The draws below stay inside these ranges and needn't reach their ends.
All inputs are finite; a program needn't handle non-finite values.
Results may differ from the reference program's by a relative error of at most 0.02.
Values may be sent and summed in bfloat16 or wider, within the bound.
A program may use at most 64 MiB of HBM per device.

```python
import jax
import jax.numpy as jnp
from jax import lax

D = 1024
CHANNELS = 512
TAPS = 31
LAYERS = 4
SEQS = 4
TOKENS = 512


def level_of(stream_key, dims, shards, low, top_value):
    level = 1.0
    for axis_at, shards_of in shards:
        heights = jax.random.uniform(jax.random.fold_in(jax.random.fold_in(stream_key, 6), axis_at), (shards_of,), jnp.float32, low / len(shards), top_value / len(shards))
        level = level * jnp.repeat(jnp.exp(heights), dims[axis_at] // shards_of).reshape((-1,) + (1,) * (len(dims) - 1 - axis_at))
    return level


def normal_values(own_key, shape, scale, most, shards=(), dtype=jnp.bfloat16):
    result = scale * jax.random.normal(own_key, shape, jnp.float32)
    if shards:
        result = result * level_of(own_key, shape, shards, -0.22, 0.18)
    return jnp.clip(result, -most, most).astype(dtype)


def setup_inputs(seed: int = 0) -> dict:
    splits = jax.random.split(jax.random.key(seed), 10)
    tokens = normal_values(splits[0], (SEQS, TOKENS, D), 1.0, 6.0, ((1, 8), (2, 4)))
    norm_gain = jnp.clip(1.0 + 0.18 * jax.random.normal(splits[1], (LAYERS, D), jnp.float32), 0.1, 1.9)
    val_weight = normal_values(splits[2], (LAYERS, D, CHANNELS), D ** -0.5, 0.1875, ((1, 8), (2, 4)))
    gate_weight = normal_values(splits[3], (LAYERS, D, CHANNELS), D ** -0.5, 0.1875, ((1, 8), (2, 4)))
    conv_taps = normal_values(splits[4], (LAYERS, TAPS, CHANNELS), TAPS ** -0.5, 1.0, ((2, 4),), jnp.float32)
    conv_bias = normal_values(splits[5], (LAYERS, CHANNELS), 0.5, 3.0, ((1, 4),), jnp.float32)
    ln_gain = jnp.clip(1.0 + 0.18 * jax.random.normal(splits[6], (LAYERS, CHANNELS), jnp.float32), 0.1, 1.9)
    ln_shift = normal_values(splits[7], (LAYERS, CHANNELS), 0.5, 3.0, ((1, 4),), jnp.float32)
    out_weight = normal_values(splits[8], (LAYERS, CHANNELS, D), CHANNELS ** -0.5, 0.25, ((1, 4), (2, 8)))
    return {"tokens": tokens, "norm_gain": norm_gain, "val_weight": val_weight, "gate_weight": gate_weight, "conv_taps": conv_taps, "conv_bias": conv_bias, "ln_gain": ln_gain, "ln_shift": ln_shift, "out_weight": out_weight}


epsilon = 1e-06

def depthwise(padded, tap_weights, length):
    running = padded[:, 0:length] * tap_weights[0]
    for tap_idx in range(1, tap_weights.shape[0]):
        running = running + padded[:, tap_idx:tap_idx + length] * tap_weights[tap_idx]
    return running

def reference(tokens, norm_gain, val_weight, gate_weight, conv_taps, conv_bias, ln_gain, ln_shift, out_weight):
    stream = tokens
    half_width = TAPS // 2
    for layer_idx in range(LAYERS):
        widened = stream.astype(jnp.float32)
        scaled = widened * jax.lax.rsqrt(lax.optimization_barrier(jnp.mean(widened * widened, axis=-1, keepdims=True)) + epsilon)
        normed = (scaled * norm_gain[layer_idx]).astype(jnp.bfloat16)
        tok_rows = normed.reshape(-1, D)
        values = jnp.dot(tok_rows, val_weight[layer_idx], preferred_element_type=jnp.float32)
        gates = jnp.dot(tok_rows, gate_weight[layer_idx], preferred_element_type=jnp.float32)
        gated = (values * jax.nn.sigmoid(gates)).astype(jnp.bfloat16).reshape(SEQS, TOKENS, CHANNELS)
        padded = jnp.pad(gated.astype(jnp.float32), ((0, 0), (half_width, half_width), (0, 0)))
        convolved = depthwise(padded, conv_taps[layer_idx], TOKENS) + conv_bias[layer_idx]
        mean_val = lax.optimization_barrier(jnp.mean(convolved, axis=-1, keepdims=True))
        centered = convolved - mean_val
        spread = lax.optimization_barrier(jnp.mean(centered * centered, axis=-1, keepdims=True))
        normalized = centered * jax.lax.rsqrt(spread + epsilon) * ln_gain[layer_idx] + ln_shift[layer_idx]
        activated = jax.nn.silu(normalized).astype(jnp.bfloat16).reshape(-1, CHANNELS)
        branch = jnp.dot(activated, out_weight[layer_idx], preferred_element_type=jnp.float32)
        stream = (stream.astype(jnp.float32) + branch.reshape(SEQS, TOKENS, D)).astype(jnp.bfloat16)
    return stream
```

```python
from functools import partial

import jax
import jax.numpy as jnp
from jax import lax
from jax.experimental import pallas as pl
from jax.experimental.pallas import tpu as pltpu
from jax.sharding import PartitionSpec as P

MESH = pl.DeviceIdType.MESH

LAYERS = 4


epsilon = 1e-06


def over_all(shard, axis, dim, absorb, state):
    everything = jax.tree.map(lambda a: lax.all_gather(a, axis, axis=dim, tiled=True), shard)
    return absorb(state, everything, jnp.int32(0))


def with_halo(shard, sides, width, wrap):
    for axis, dim in sides:
        size, length = lax.axis_size(axis), shard.shape[dim]
        up = [(i, (i + 1) % size) for i in range(size if wrap else size - 1)]
        down = [(j, i) for i, j in up]
        last = lax.slice_in_dim(shard, length - width, length, axis=dim)
        initial = lax.slice_in_dim(shard, 0, width, axis=dim)
        before = lax.ppermute(last, axis, up)
        after = lax.ppermute(initial, axis, down)
        shard = jnp.concatenate([before, shard, after], axis=dim)
    return shard


def over_all_2(shard, axis, dim, work):
    return work(lax.all_gather(shard, axis, axis=dim, tiled=True), jnp.int32(0))


def depthwise(padded, tap_weights, length):
    running = padded[:, 0:length] * tap_weights[0]
    for tap_idx in range(1, tap_weights.shape[0]):
        running = running + padded[:, tap_idx : tap_idx + length] * tap_weights[tap_idx]
    return running


def add_rows(left_rows, running, shard_piece, offset):
    columns = lax.dynamic_slice_in_dim(left_rows, offset, shard_piece.shape[0], 1)
    return running + jnp.dot(columns, shard_piece, preferred_element_type=jnp.float32)


def project_rows(left_rows, shard_piece, offset):
    return jnp.dot(left_rows, shard_piece, preferred_element_type=jnp.float32)


def shards(
    tokens, norm_gain, val_weight, gate_weight, conv_taps, conv_bias, ln_gain, ln_shift, out_weight
):
    stream = tokens
    num_seqs = tokens.shape[0]
    local_len = tokens.shape[1]
    chan_width = val_weight.shape[2]
    all_channels = chan_width * lax.axis_size("tp")
    half_width = conv_taps.shape[1] // 2
    for layer_idx in range(LAYERS):
        gathered = lax.all_gather(stream, "tp", axis=2, tiled=True)
        widened = gathered.astype(jnp.float32)
        scaled = widened * lax.rsqrt(jnp.mean(widened * widened, axis=-1, keepdims=True) + epsilon)
        normed = (scaled * norm_gain[layer_idx]).astype(jnp.bfloat16)
        tok_rows = normed.reshape(-1, normed.shape[2])
        zeroed = jnp.zeros((tok_rows.shape[0], chan_width), jnp.float32)
        values = over_all(val_weight[layer_idx], "sp", 0, partial(add_rows, tok_rows), zeroed)
        gates = over_all(gate_weight[layer_idx], "sp", 0, partial(add_rows, tok_rows), zeroed)
        gated = (
            (values * jax.nn.sigmoid(gates))
            .astype(jnp.bfloat16)
            .reshape(num_seqs, local_len, chan_width)
        )
        padded = with_halo(gated, (("sp", 1),), half_width, False)
        convolved = (
            depthwise(padded.astype(jnp.float32), conv_taps[layer_idx], local_len)
            + conv_bias[layer_idx]
        )
        first_sum, second_sum = lax.psum(
            (jnp.sum(convolved, axis=-1), jnp.sum(convolved * convolved, axis=-1)), "tp"
        )
        mean_val = (first_sum / all_channels)[..., None]
        spread = (second_sum / all_channels)[..., None] - mean_val * mean_val
        centered = convolved - mean_val
        normalized = (
            centered * lax.rsqrt(spread + epsilon) * ln_gain[layer_idx] + ln_shift[layer_idx]
        )
        activated = jax.nn.silu(normalized).astype(jnp.bfloat16).reshape(-1, chan_width)
        partial_terms = over_all_2(out_weight[layer_idx], "sp", 1, partial(project_rows, activated))
        full_width = partial_terms.shape[1]
        summed = lax.psum_scatter(
            partial_terms.reshape(num_seqs, local_len, full_width).astype(jnp.bfloat16),
            "tp",
            scatter_dimension=2,
            tiled=True,
        ).astype(jnp.float32)
        stream = (stream.astype(jnp.float32) + summed).astype(jnp.bfloat16)
    return stream


def stack_kernel(
    dims, tok, gain, val_w, gate_w, taps, bias, lng, lns, out_w, out,
    xs, vals, gates, outs, ptaps, pbias, plng, plns, gs, cv, act, stage,
    loc_sem, tsend, trecv, psend, precv, wsend, wrecv, osend, orecv,
):
    SP, TP, Z, L, D, C, F, W, K, TAPS, PAD, E = dims
    sp, tp = lax.axis_index("sp"), lax.axis_index("tp")
    zi, yi, xi, ci = sp // 2, sp % 2, tp // 2, tp % 2
    half = TAPS // 2

    def remote(src, dst, ss, rs, to_sp, to_tp):
        return pltpu.make_async_remote_copy(
            src_ref=src, dst_ref=dst, send_sem=ss, recv_sem=rs,
            device_id=(to_sp, to_tp), device_id_type=MESH,
        )

    def feat(t):
        return pl.ds(pl.multiple_of(t * F, F), F)

    finish = []

    def tok_copy(side, d, to_sp):
        to = lax.rem(tp + d, TP)
        rows = {0: (0, L, E), 1: (L - E, E, 0), 2: (0, E, E + L)}[side]
        return remote(
            tok.at[to, pl.ds(rows[0], rows[1]), :],
            xs.at[pl.ds(rows[2], rows[1]), feat(tp)],
            tsend.at[side, d], trecv.at[side, d], to_sp, to,
        )

    own_tok = pltpu.make_async_copy(tok.at[tp], xs.at[pl.ds(E, L), feat(tp)], loc_sem.at[0])
    own_tok.start()

    @pl.when(sp == 0)
    def _():
        xs[pl.ds(0, E), :] = jnp.zeros((E, D), xs.dtype)

    @pl.when(sp == SP - 1)
    def _():
        xs[pl.ds(E + L, E), :] = jnp.zeros((E, D), xs.dtype)

    sources = (val_w, gate_w, out_w)
    bufs = (vals, gates, outs)
    units = [(l, k) for l in range(LAYERS) for k in range(3)]

    def block(n, zs, ys, t):
        l, k = units[n]
        part = pl.ds(pl.multiple_of(t * W, W), W)
        if k < 2:
            return bufs[k].at[l, zs, ys, :, part]
        return bufs[k].at[l, zs, ys, part, :]

    every = slice(None)
    sib, xpeer = xi * 2 + (1 - ci), (1 - xi) * 2 + ci
    ypeer = zi * 2 + (1 - yi)

    def y_first(n):
        l, k = units[n]
        return k == 0 or (k == 2 and l % 2 == 0)

    own = []
    first = []
    for n, (l, k) in enumerate(units):
        c = pltpu.make_async_copy(sources[k].at[l], block(n, zi, yi, tp), loc_sem.at[1 + n])
        own.append(c)
        first.append([
            remote(
                sources[k].at[l], block(n, zi, yi, tp),
                wsend.at[n, d - 1], wrecv.at[n, d - 1], lax.rem(zi + d, Z) * 2 + yi, tp,
            )
            for d in range(1, Z)
        ])

    def start(n, slot, zs, ys, t, to_sp, to_tp):
        ref = block(n, zs, ys, t)
        c = remote(ref, ref, wsend.at[n, slot], wrecv.at[n, slot], to_sp, to_tp)
        c.start()
        finish.append(c)
        return c

    for c in own[:2]:
        c.start()
    for n in range(2):
        for c in first[n]:
            c.start()
    for d in range(1, TP):
        tok_copy(0, d, sp).start()
    small, params = [], []
    for i, (src, dst) in enumerate(((taps, ptaps), (bias, pbias), (lng, plng), (lns, plns))):
        c = pltpu.make_async_copy(src, dst.at[tp], loc_sem.at[1 + len(units) + i])
        c.start()
        small.append(c)
        for d in range(1, TP):
            r = remote(src, dst.at[tp], psend.at[i, d], precv.at[i, d], sp, lax.rem(tp + d, TP))
            r.start()
            finish.append(r)
            params.append(r)

    @pl.when(sp < SP - 1)
    def _():
        for d in range(TP):
            tok_copy(1, d, sp + 1).start()

    @pl.when(sp > 0)
    def _():
        for d in range(TP):
            tok_copy(2, d, sp - 1).start()

    for n in range(2, len(units)):
        own[n].start()
        for c in first[n]:
            c.start()

    z0 = Z - 1
    hold = {}

    def step2(n):
        own[n].wait()
        for c in first[n]:
            c.wait_recv()
            finish.append(c)
        if y_first(n):
            hold[n] = [start(n, z0, every, yi, tp, ypeer, tp)]
        else:
            hold[n] = [start(n, z0, every, yi, tp, sp, xpeer)]
        hold[n, "s"] = [start(n, z0 + 1, every, yi, tp, sp, sib)]

    def step3(n):
        for c in hold[n]:
            c.wait_recv()
        if y_first(n):
            hold[n] = [start(n, z0 + 2, every, every, tp, sp, xpeer)]
            hold[n, "s"].append(start(n, z0 + 3, every, 1 - yi, tp, sp, sib))
        else:
            hold[n] = [
                start(n, z0 + 2, every, yi, tp, ypeer, tp),
                start(n, z0 + 4, every, yi, xpeer, ypeer, tp),
            ]
            hold[n, "s"].append(start(n, z0 + 3, every, yi, xpeer, sp, sib))

    def step4(n):
        for c in hold[n]:
            c.wait_recv()
        if y_first(n):
            hold[n, "s"].append(start(n, z0 + 5, every, every, xpeer, sp, sib))
        else:
            hold[n, "s"].append(start(n, z0 + 5, every, 1 - yi, tp, sp, sib))
            hold[n, "s"].append(start(n, z0 + 6, every, 1 - yi, xpeer, sp, sib))

    def step5(n):
        for c in hold[n, "s"]:
            c.wait_recv()

    def tick(t):
        for lag, step in enumerate((step2, step3, step4, step5)):
            if 0 <= t - lag < len(units):
                step(t - lag)

    NC = C // 128

    def gated_part(l):
        rows, base = L + 2 * E - 2 * PAD * l, PAD * l
        x = xs[pl.ds(base, rows), :].astype(jnp.float32)
        scaled = x * lax.rsqrt(jnp.mean(x * x, axis=-1, keepdims=True) + epsilon)
        normed = (scaled * gain[pl.ds(l, 1), :]).astype(jnp.bfloat16)
        place = sp * L - E + base + lax.broadcasted_iota(jnp.int32, (rows, 256), 0)
        inside = (place >= 0) & (place < SP * L)
        for j in range(C // 256):
            cols = pl.ds(j * 256, 256)
            v = jnp.dot(normed, vals[l, :, :, :, cols].reshape(D, 256), preferred_element_type=jnp.float32)
            g = jnp.dot(normed, gates[l, :, :, :, cols].reshape(D, 256), preferred_element_type=jnp.float32)
            r = (v * jax.nn.sigmoid(g)).astype(jnp.bfloat16).astype(jnp.float32)
            r = jnp.where(inside, r, 0.0)
            gs[2 * j, pl.ds(0, rows), :] = r[:, :128]
            gs[2 * j + 1, pl.ds(0, rows), :] = r[:, 128:]

    def conv_part(l):
        rows = L + 2 * E - 2 * PAD * (l + 1)

        per = W // 128

        def one(c, carry):
            t = c // per
            lane = pl.ds(pl.multiple_of((c % per) * 128, 128), 128) if per > 1 else slice(None)
            acc = gs[c, pl.ds(PAD - half, rows), :] * ptaps[t, l, pl.ds(0, 1), lane]
            for k in range(1, TAPS):
                acc = acc + gs[c, pl.ds(PAD - half + k, rows), :] * ptaps[t, l, pl.ds(k, 1), lane]
            cv[c, pl.ds(0, rows), :] = acc + pbias[t, pl.ds(l, 1), lane]
            return carry

        lax.fori_loop(0, NC, one, 0)
        parts = [cv[c, pl.ds(0, rows), :] for c in range(NC)]
        mean = jnp.sum(sum(parts[1:], parts[0]), axis=-1, keepdims=True) / C
        cent = [p - mean for p in parts]
        sq = [p * p for p in cent]
        inv = lax.rsqrt(jnp.sum(sum(sq[1:], sq[0]), axis=-1, keepdims=True) / C + epsilon)
        for c in range(NC):
            t, lane = c // per, pl.ds((c % per) * 128, 128)
            y = cent[c] * inv * plng[t, pl.ds(l, 1), lane] + plns[t, pl.ds(l, 1), lane]
            act[pl.ds(0, rows), pl.ds(c * 128, 128)] = (y * jax.nn.sigmoid(y)).astype(jnp.bfloat16)

    def out_part(l):
        rows, base = L + 2 * E - 2 * PAD * (l + 1), PAD * (l + 1)
        a = act[pl.ds(0, rows), :]
        for z in range(Z):
            w = jnp.concatenate([outs[l, z, 0], outs[l, z, 1]], axis=1)
            y = jnp.dot(a, w, preferred_element_type=jnp.float32)
            cols = pl.ds(z * 2 * K, 2 * K)
            s = xs[pl.ds(base, rows), cols].astype(jnp.float32)
            xs[pl.ds(base, rows), cols] = (s + y).astype(jnp.bfloat16)

    for t in range(4):
        tick(t)
    own_tok.wait()
    for d in range(1, TP):
        c = tok_copy(0, d, sp)
        c.wait_recv()
        finish.append(c)
    for c in small:
        c.wait()
    for c in params:
        c.wait_recv()

    @pl.when(sp > 0)
    def _():
        for d in range(TP):
            tok_copy(1, d, sp).wait_recv()

    @pl.when(sp < SP - 1)
    def _():
        for d in range(TP):
            tok_copy(2, d, sp).wait_recv()

    t = 4
    for l in range(LAYERS):
        while t <= 3 * l + 4:
            tick(t)
            t += 1
        gated_part(l)
        tick(t)
        t += 1
        conv_part(l)
        out_part(l)

    sends = []
    for d in range(1, TP):
        to = lax.rem(tp + d, TP)
        c = remote(
            xs.at[pl.ds(E, L), feat(to)], out.at[tp],
            osend.at[d], orecv.at[d], sp, to,
        )
        c.start()
        sends.append(c)
    mine = pltpu.make_async_copy(xs.at[pl.ds(E, L), feat(tp)], out.at[tp], loc_sem.at[0])
    mine.start()
    for c in finish:
        c.wait_send()

    @pl.when(sp < SP - 1)
    def _():
        for d in range(TP):
            tok_copy(1, d, sp).wait_send()

    @pl.when(sp > 0)
    def _():
        for d in range(TP):
            tok_copy(2, d, sp).wait_send()

    mine.wait()
    for c in sends:
        c.wait()


def stacked(tokens, norm_gain, val_weight, gate_weight, conv_taps, conv_bias, ln_gain, ln_shift, out_weight):
    SP, TP = lax.axis_size("sp"), lax.axis_size("tp")
    seqs, L, F = tokens.shape
    D = F * TP
    layers, K, W = val_weight.shape
    C = W * TP
    TAPS = conv_taps.shape[1]
    PAD = -(-(TAPS // 2) // 16) * 16
    E = PAD * LAYERS
    Z = SP // 2
    rows = L + 2 * E
    vmem = pl.BlockSpec(memory_space=pltpu.VMEM)
    bf16, f32 = jnp.bfloat16, jnp.float32
    dma = pltpu.SemaphoreType.DMA
    units = 3 * LAYERS
    return pl.pallas_call(
        partial(stack_kernel, (SP, TP, Z, L, D, C, F, W, K, TAPS, PAD, E)),
        out_shape=jax.ShapeDtypeStruct(tokens.shape, tokens.dtype),
        in_specs=[vmem] * 9,
        out_specs=vmem,
        scratch_shapes=[
            pltpu.VMEM((rows, D), bf16),
            pltpu.VMEM((LAYERS, Z, 2, K, C), bf16),
            pltpu.VMEM((LAYERS, Z, 2, K, C), bf16),
            pltpu.VMEM((LAYERS, Z, 2, C, K), bf16),
            pltpu.VMEM((TP,) + conv_taps.shape, f32),
            pltpu.VMEM((TP,) + conv_bias.shape, f32),
            pltpu.VMEM((TP,) + conv_bias.shape, f32),
            pltpu.VMEM((TP,) + conv_bias.shape, f32),
            pltpu.VMEM((C // 128, rows, 128), f32),
            pltpu.VMEM((C // 128, rows, 128), f32),
            pltpu.VMEM((rows, C), bf16),
            pltpu.VMEM((8, 128), f32),
            dma((1 + units + 4,)),
            dma((3, TP)), dma((3, TP)),
            dma((4, TP)), dma((4, TP)),
            dma((units, Z + 6)), dma((units, Z + 6)),
            dma((TP,)), dma((TP,)),
        ],
        compiler_params=pltpu.CompilerParams(has_side_effects=True, vmem_limit_bytes=48 * 1024 * 1024),
        name="stack",
    )(tokens, norm_gain, val_weight, gate_weight, conv_taps, conv_bias, ln_gain, ln_shift, out_weight)


def fits(tokens, val_weight, conv_taps):
    SP, TP = lax.axis_size("sp"), lax.axis_size("tp")
    seqs, L, F = tokens.shape
    layers, K, W = val_weight.shape
    halo = -(-(conv_taps.shape[1] // 2) // 16) * 16 * LAYERS
    return (
        TP == 4 and SP % 2 == 0 and seqs == TP and L >= halo and L % 16 == 0
        and F % 128 == 0 and K % 128 == 0 and W % 128 == 0 and layers == LAYERS
    )


def either(tokens, norm_gain, val_weight, gate_weight, conv_taps, *rest):
    work = stacked if fits(tokens, val_weight, conv_taps) else shards
    return work(tokens, norm_gain, val_weight, gate_weight, conv_taps, *rest)


def solution(mesh):
    placed = (
        P(None, "sp", "tp"),
        P(),
        P(None, "sp", "tp"),
        P(None, "sp", "tp"),
        P(None, None, "tp"),
        P(None, "tp"),
        P(None, "tp"),
        P(None, "tp"),
        P(None, "tp", "sp"),
    )
    return jax.shard_map(
        either, mesh=mesh, in_specs=placed, out_specs=P(None, "sp", "tp"), check_vma=False
    )
```

```python
from functools import partial

import jax
import jax.numpy as jnp
from jax import lax
from jax.experimental import pallas as pl
from jax.experimental.pallas import tpu as pltpu
from jax.sharding import PartitionSpec as P

MESH = pl.DeviceIdType.MESH

LAYERS = 4
LAGS = (0, 1, 2, 3)


epsilon = 1e-06


def over_all(shard, axis, dim, absorb, state):
    everything = jax.tree.map(lambda a: lax.all_gather(a, axis, axis=dim, tiled=True), shard)
    return absorb(state, everything, jnp.int32(0))


def with_halo(shard, sides, width, wrap):
    for axis, dim in sides:
        size, length = lax.axis_size(axis), shard.shape[dim]
        up = [(i, (i + 1) % size) for i in range(size if wrap else size - 1)]
        down = [(j, i) for i, j in up]
        last = lax.slice_in_dim(shard, length - width, length, axis=dim)
        initial = lax.slice_in_dim(shard, 0, width, axis=dim)
        before = lax.ppermute(last, axis, up)
        after = lax.ppermute(initial, axis, down)
        shard = jnp.concatenate([before, shard, after], axis=dim)
    return shard


def over_all_2(shard, axis, dim, work):
    return work(lax.all_gather(shard, axis, axis=dim, tiled=True), jnp.int32(0))


def depthwise(padded, tap_weights, length):
    running = padded[:, 0:length] * tap_weights[0]
    for tap_idx in range(1, tap_weights.shape[0]):
        running = running + padded[:, tap_idx : tap_idx + length] * tap_weights[tap_idx]
    return running


def add_rows(left_rows, running, shard_piece, offset):
    columns = lax.dynamic_slice_in_dim(left_rows, offset, shard_piece.shape[0], 1)
    return running + jnp.dot(columns, shard_piece, preferred_element_type=jnp.float32)


def project_rows(left_rows, shard_piece, offset):
    return jnp.dot(left_rows, shard_piece, preferred_element_type=jnp.float32)


def shards(
    tokens, norm_gain, val_weight, gate_weight, conv_taps, conv_bias, ln_gain, ln_shift, out_weight
):
    stream = tokens
    num_seqs = tokens.shape[0]
    local_len = tokens.shape[1]
    chan_width = val_weight.shape[2]
    all_channels = chan_width * lax.axis_size("tp")
    half_width = conv_taps.shape[1] // 2
    for layer_idx in range(LAYERS):
        gathered = lax.all_gather(stream, "tp", axis=2, tiled=True)
        widened = gathered.astype(jnp.float32)
        scaled = widened * lax.rsqrt(jnp.mean(widened * widened, axis=-1, keepdims=True) + epsilon)
        normed = (scaled * norm_gain[layer_idx]).astype(jnp.bfloat16)
        tok_rows = normed.reshape(-1, normed.shape[2])
        zeroed = jnp.zeros((tok_rows.shape[0], chan_width), jnp.float32)
        values = over_all(val_weight[layer_idx], "sp", 0, partial(add_rows, tok_rows), zeroed)
        gates = over_all(gate_weight[layer_idx], "sp", 0, partial(add_rows, tok_rows), zeroed)
        gated = (
            (values * jax.nn.sigmoid(gates))
            .astype(jnp.bfloat16)
            .reshape(num_seqs, local_len, chan_width)
        )
        padded = with_halo(gated, (("sp", 1),), half_width, False)
        convolved = (
            depthwise(padded.astype(jnp.float32), conv_taps[layer_idx], local_len)
            + conv_bias[layer_idx]
        )
        first_sum, second_sum = lax.psum(
            (jnp.sum(convolved, axis=-1), jnp.sum(convolved * convolved, axis=-1)), "tp"
        )
        mean_val = (first_sum / all_channels)[..., None]
        spread = (second_sum / all_channels)[..., None] - mean_val * mean_val
        centered = convolved - mean_val
        normalized = (
            centered * lax.rsqrt(spread + epsilon) * ln_gain[layer_idx] + ln_shift[layer_idx]
        )
        activated = jax.nn.silu(normalized).astype(jnp.bfloat16).reshape(-1, chan_width)
        partial_terms = over_all_2(out_weight[layer_idx], "sp", 1, partial(project_rows, activated))
        full_width = partial_terms.shape[1]
        summed = lax.psum_scatter(
            partial_terms.reshape(num_seqs, local_len, full_width).astype(jnp.bfloat16),
            "tp",
            scatter_dimension=2,
            tiled=True,
        ).astype(jnp.float32)
        stream = (stream.astype(jnp.float32) + summed).astype(jnp.bfloat16)
    return stream


def stack_kernel(
    dims, tok, gain, val_w, gate_w, taps, bias, lng, lns, out_w, out,
    xs, vals, gates, outs, ptaps, pbias, plng, plns, gs, cv, act, stage,
    loc_sem, tsend, trecv, psend, precv, wsend, wrecv, osend, orecv,
):
    SP, TP, Z, L, D, C, F, W, K, TAPS, PAD, E = dims
    sp, tp = lax.axis_index("sp"), lax.axis_index("tp")
    zi, yi, xi, ci = sp // 2, sp % 2, tp // 2, tp % 2
    half = TAPS // 2

    def remote(src, dst, ss, rs, to_sp, to_tp):
        return pltpu.make_async_remote_copy(
            src_ref=src, dst_ref=dst, send_sem=ss, recv_sem=rs,
            device_id=(to_sp, to_tp), device_id_type=MESH,
        )

    def feat(t):
        return pl.ds(pl.multiple_of(t * F, F), F)

    finish = []

    def tok_copy(side, d, to_sp):
        to = lax.rem(tp + d, TP)
        rows = {0: (0, L, E), 1: (L - E, E, 0), 2: (0, E, E + L)}[side]
        return remote(
            tok.at[to, pl.ds(rows[0], rows[1]), :],
            xs.at[pl.ds(rows[2], rows[1]), feat(tp)],
            tsend.at[side, d], trecv.at[side, d], to_sp, to,
        )

    own_tok = pltpu.make_async_copy(tok.at[tp], xs.at[pl.ds(E, L), feat(tp)], loc_sem.at[0])
    own_tok.start()

    @pl.when(sp == 0)
    def _():
        xs[pl.ds(0, E), :] = jnp.zeros((E, D), xs.dtype)

    @pl.when(sp == SP - 1)
    def _():
        xs[pl.ds(E + L, E), :] = jnp.zeros((E, D), xs.dtype)

    sources = (val_w, gate_w, out_w)
    bufs = (vals, gates, outs)
    units = [(l, k, h) for l in range(LAYERS) for k in range(3) for h in range(2)]

    def block(n, zs, ys, t):
        l, k, h = units[n]
        if k < 2:
            return bufs[k].at[l, zs, ys, t, pl.ds(h * (K // 2), K // 2), :]
        rows = pl.ds(pl.multiple_of(t * W + h * (W // 2), W // 2), W // 2)
        return bufs[k].at[l, zs, ys, rows, :]

    def source(n):
        l, k, h = units[n]
        rows = sources[k].shape[1] // 2
        return sources[k].at[l, pl.ds(h * rows, rows), :]

    every = slice(None)
    sib, xpeer = xi * 2 + (1 - ci), (1 - xi) * 2 + ci
    ypeer = zi * 2 + (1 - yi)

    def y_first(n):
        return units[n][2] == 0

    own = []
    first = []
    for n in range(len(units)):
        c = pltpu.make_async_copy(source(n), block(n, zi, yi, tp), loc_sem.at[1 + n])
        own.append(c)
        first.append([
            remote(
                source(n), block(n, zi, yi, tp),
                wsend.at[n, d - 1], wrecv.at[n, d - 1], lax.rem(zi + d, Z) * 2 + yi, tp,
            )
            for d in range(1, Z)
        ])

    def start(n, slot, zs, ys, t, to_sp, to_tp):
        ref = block(n, zs, ys, t)
        c = remote(ref, ref, wsend.at[n, slot], wrecv.at[n, slot], to_sp, to_tp)
        c.start()
        finish.append(c)
        return c

    for c in own[:4]:
        c.start()
    for n in range(4):
        for c in first[n]:
            c.start()
    for d in range(1, TP):
        tok_copy(0, d, sp).start()
    small, params = [], []
    for i, (src, dst) in enumerate(((taps, ptaps), (bias, pbias), (lng, plng), (lns, plns))):
        c = pltpu.make_async_copy(src, dst.at[tp], loc_sem.at[1 + len(units) + i])
        c.start()
        small.append(c)
        for d in range(1, TP):
            r = remote(src, dst.at[tp], psend.at[i, d], precv.at[i, d], sp, lax.rem(tp + d, TP))
            r.start()
            finish.append(r)
            params.append(r)

    @pl.when(sp < SP - 1)
    def _():
        for d in range(TP):
            tok_copy(1, d, sp + 1).start()

    @pl.when(sp > 0)
    def _():
        for d in range(TP):
            tok_copy(2, d, sp - 1).start()

    for n in range(4, len(units)):
        own[n].start()
        for c in first[n]:
            c.start()

    z0 = Z - 1
    hold = {}

    def step2(n):
        own[n].wait()
        for c in first[n]:
            c.wait_recv()
            finish.append(c)
        if y_first(n):
            hold[n] = [start(n, z0, every, yi, tp, ypeer, tp)]
        else:
            hold[n] = [start(n, z0, every, yi, tp, sp, xpeer)]
        hold[n, "s"] = [start(n, z0 + 1, every, yi, tp, sp, sib)]

    def step3(n):
        for c in hold[n]:
            c.wait_recv()
        if y_first(n):
            hold[n] = [start(n, z0 + 2, every, every, tp, sp, xpeer)]
            hold[n, "s"].append(start(n, z0 + 3, every, 1 - yi, tp, sp, sib))
        else:
            hold[n] = [
                start(n, z0 + 2, every, yi, tp, ypeer, tp),
                start(n, z0 + 4, every, yi, xpeer, ypeer, tp),
            ]
            hold[n, "s"].append(start(n, z0 + 3, every, yi, xpeer, sp, sib))

    def step4(n):
        for c in hold[n]:
            c.wait_recv()
        if y_first(n):
            hold[n, "s"].append(start(n, z0 + 5, every, every, xpeer, sp, sib))
        else:
            hold[n, "s"].append(start(n, z0 + 5, every, 1 - yi, tp, sp, sib))
            hold[n, "s"].append(start(n, z0 + 6, every, 1 - yi, xpeer, sp, sib))

    def step5(n):
        for c in hold[n, "s"]:
            c.wait_recv()

    def tick(t):
        for lag, step in zip(LAGS, (step2, step3, step4, step5)):
            for h in range(2):
                if 0 <= t - lag < len(units) // 2:
                    step(2 * (t - lag) + h)

    NC = C // 128

    def gated_part(l):
        rows, base = L + 2 * E - 2 * PAD * l, PAD * l
        x = xs[pl.ds(base, rows), :].astype(jnp.float32)
        scaled = x * lax.rsqrt(jnp.mean(x * x, axis=-1, keepdims=True) + epsilon)
        normed = (scaled * gain[pl.ds(l, 1), :]).astype(jnp.bfloat16)
        place = sp * L - E + base + lax.broadcasted_iota(jnp.int32, (rows, 256), 0)
        inside = (place >= 0) & (place < SP * L)
        for j in range(C // 256):
            vw, gw = (
                jnp.concatenate([b[l, :, :, 2 * j + i].reshape(D, W) for i in range(2)], axis=1)
                for b in (vals, gates)
            )
            v = jnp.dot(normed, vw, preferred_element_type=jnp.float32)
            g = jnp.dot(normed, gw, preferred_element_type=jnp.float32)
            r = (v * jax.nn.sigmoid(g)).astype(jnp.bfloat16).astype(jnp.float32)
            r = jnp.where(inside, r, 0.0)
            gs[2 * j, pl.ds(0, rows), :] = r[:, :128]
            gs[2 * j + 1, pl.ds(0, rows), :] = r[:, 128:]

    def conv_part(l):
        rows = L + 2 * E - 2 * PAD * (l + 1)

        per = W // 128

        def one(c, carry):
            t = c // per
            lane = pl.ds(pl.multiple_of((c % per) * 128, 128), 128) if per > 1 else slice(None)
            acc = gs[c, pl.ds(PAD - half, rows), :] * ptaps[t, l, pl.ds(0, 1), lane]
            for k in range(1, TAPS):
                acc = acc + gs[c, pl.ds(PAD - half + k, rows), :] * ptaps[t, l, pl.ds(k, 1), lane]
            cv[c, pl.ds(0, rows), :] = acc + pbias[t, pl.ds(l, 1), lane]
            return carry

        lax.fori_loop(0, NC, one, 0)
        parts = [cv[c, pl.ds(0, rows), :] for c in range(NC)]
        mean = jnp.sum(sum(parts[1:], parts[0]), axis=-1, keepdims=True) / C
        cent = [p - mean for p in parts]
        sq = [p * p for p in cent]
        inv = lax.rsqrt(jnp.sum(sum(sq[1:], sq[0]), axis=-1, keepdims=True) / C + epsilon)
        for c in range(NC):
            t, lane = c // per, pl.ds((c % per) * 128, 128)
            y = cent[c] * inv * plng[t, pl.ds(l, 1), lane] + plns[t, pl.ds(l, 1), lane]
            act[pl.ds(0, rows), pl.ds(c * 128, 128)] = (y * jax.nn.sigmoid(y)).astype(jnp.bfloat16)

    def out_part(l):
        rows, base = L + 2 * E - 2 * PAD * (l + 1), PAD * (l + 1)
        a = act[pl.ds(0, rows), :]
        for z in range(Z):
            w = jnp.concatenate([outs[l, z, 0], outs[l, z, 1]], axis=1)
            y = jnp.dot(a, w, preferred_element_type=jnp.float32)
            cols = pl.ds(z * 2 * K, 2 * K)
            s = xs[pl.ds(base, rows), cols].astype(jnp.float32)
            xs[pl.ds(base, rows), cols] = (s + y).astype(jnp.bfloat16)

    def arrived():
        own_tok.wait()
        for d in range(1, TP):
            c = tok_copy(0, d, sp)
            c.wait_recv()
            finish.append(c)
        for c in small:
            c.wait()
        for c in params:
            c.wait_recv()

        @pl.when(sp > 0)
        def _():
            for d in range(TP):
                tok_copy(1, d, sp).wait_recv()

        @pl.when(sp < SP - 1)
        def _():
            for d in range(TP):
                tok_copy(2, d, sp).wait_recv()

    t, last = 0, LAGS[-1]
    for l in range(LAYERS):
        while t <= 3 * l + 1 + last:
            tick(t)
            t += 1
        if l == 0:
            arrived()
        gated_part(l)
        tick(t)
        t += 1
        conv_part(l)
        if l + 1 < LAYERS:
            tick(t)
            t += 1
        out_part(l)

    sends = []
    for d in range(1, TP):
        to = lax.rem(tp + d, TP)
        c = remote(
            xs.at[pl.ds(E, L), feat(to)], out.at[tp],
            osend.at[d], orecv.at[d], sp, to,
        )
        c.start()
        sends.append(c)
    mine = pltpu.make_async_copy(xs.at[pl.ds(E, L), feat(tp)], out.at[tp], loc_sem.at[0])
    mine.start()
    for c in finish:
        c.wait_send()

    @pl.when(sp < SP - 1)
    def _():
        for d in range(TP):
            tok_copy(1, d, sp).wait_send()

    @pl.when(sp > 0)
    def _():
        for d in range(TP):
            tok_copy(2, d, sp).wait_send()

    mine.wait()
    for c in sends:
        c.wait()


def stacked(tokens, norm_gain, val_weight, gate_weight, conv_taps, conv_bias, ln_gain, ln_shift, out_weight):
    SP, TP = lax.axis_size("sp"), lax.axis_size("tp")
    seqs, L, F = tokens.shape
    D = F * TP
    layers, K, W = val_weight.shape
    C = W * TP
    TAPS = conv_taps.shape[1]
    PAD = -(-(TAPS // 2) // 16) * 16
    E = PAD * LAYERS
    Z = SP // 2
    rows = L + 2 * E
    vmem = pl.BlockSpec(memory_space=pltpu.VMEM)
    bf16, f32 = jnp.bfloat16, jnp.float32
    dma = pltpu.SemaphoreType.DMA
    units = 6 * LAYERS
    return pl.pallas_call(
        partial(stack_kernel, (SP, TP, Z, L, D, C, F, W, K, TAPS, PAD, E)),
        out_shape=jax.ShapeDtypeStruct(tokens.shape, tokens.dtype),
        in_specs=[vmem] * 9,
        out_specs=vmem,
        scratch_shapes=[
            pltpu.VMEM((rows, D), bf16),
            pltpu.VMEM((LAYERS, Z, 2, TP, K, W), bf16),
            pltpu.VMEM((LAYERS, Z, 2, TP, K, W), bf16),
            pltpu.VMEM((LAYERS, Z, 2, C, K), bf16),
            pltpu.VMEM((TP,) + conv_taps.shape, f32),
            pltpu.VMEM((TP,) + conv_bias.shape, f32),
            pltpu.VMEM((TP,) + conv_bias.shape, f32),
            pltpu.VMEM((TP,) + conv_bias.shape, f32),
            pltpu.VMEM((C // 128, rows, 128), f32),
            pltpu.VMEM((C // 128, rows, 128), f32),
            pltpu.VMEM((rows, C), bf16),
            pltpu.VMEM((8, 128), f32),
            dma((1 + units + 4,)),
            dma((3, TP)), dma((3, TP)),
            dma((4, TP)), dma((4, TP)),
            dma((units, Z + 6)), dma((units, Z + 6)),
            dma((TP,)), dma((TP,)),
        ],
        compiler_params=pltpu.CompilerParams(has_side_effects=True, vmem_limit_bytes=48 * 1024 * 1024),
        name="stack",
    )(tokens, norm_gain, val_weight, gate_weight, conv_taps, conv_bias, ln_gain, ln_shift, out_weight)


def fits(tokens, val_weight, conv_taps):
    SP, TP = lax.axis_size("sp"), lax.axis_size("tp")
    seqs, L, F = tokens.shape
    layers, K, W = val_weight.shape
    halo = -(-(conv_taps.shape[1] // 2) // 16) * 16 * LAYERS
    return (
        TP == 4 and SP % 2 == 0 and seqs == TP and L >= halo and L % 16 == 0
        and F % 128 == 0 and K % 128 == 0 and W == 128 and layers == LAYERS
    )


def either(tokens, norm_gain, val_weight, gate_weight, conv_taps, *rest):
    work = stacked if fits(tokens, val_weight, conv_taps) else shards
    return work(tokens, norm_gain, val_weight, gate_weight, conv_taps, *rest)


def solution(mesh):
    placed = (
        P(None, "sp", "tp"),
        P(),
        P(None, "sp", "tp"),
        P(None, "sp", "tp"),
        P(None, None, "tp"),
        P(None, "tp"),
        P(None, "tp"),
        P(None, "tp"),
        P(None, "tp", "sp"),
    )
    return jax.shard_map(
        either, mesh=mesh, in_specs=placed, out_specs=P(None, "sp", "tp"), check_vma=False
    )
```
